32 devices in a mesh: dp: 4 (over y, x), kv: 4 (over z), tp: 2 (over core).
Axes of the slice: x: 2, y: 2, z: 4, core: 2. Of those that a mesh axis runs over, the one named last changes fastest.
Arguments:
- pieces: bfloat16 [4096, 8, 2048], P(('kv', 'tp'), 'dp'), parts along dimension 1, may hold values from -6 to 6
- new_tokens: bfloat16 [256, 2048], P(('dp', 'kv', 'tp')), parts along dimension 0, may hold values from -6 to 6
- w_query: bfloat16 [2048, 1024], P(None, 'tp'), may hold values from -0.125 to 0.125
- w_key: bfloat16 [2048, 1024], P(None, 'tp'), may hold values from -0.125 to 0.125
- w_value: bfloat16 [2048, 2048], P(None, 'tp'), may hold values from -0.125 to 0.125
- w_decay: bfloat16 [2048, 1024], P(None, 'tp'), may hold values from -0.125 to 0.125
- decay_bias: float32 [1024], replicated, may hold values from 0 to 9
- norm_gain: float32 [2048], replicated, may hold values from 0.1 to 1.9
- head_gain: float32 [2048], replicated, may hold values from 0.1 to 1.9
- w_out: bfloat16 [2048, 2048], replicated, may hold values from -0.125 to 0.125
- prompt_state: float32 [8, 8, 128, 256], P('dp', 'tp', 'kv'), parts along dimension 0, may hold values from -8 to 8
- decode_state: float32 [256, 8, 128, 256], P(('dp', 'kv'), 'tp'), parts along dimension 0, may hold values from -8 to 8
Outputs:
- mixed_piece: bfloat16 [4096, 8, 2048], P(('kv', 'tp'), 'dp'), parts along dimension 1
- mixed_decode: bfloat16 [256, 2048], P(('dp', 'kv', 'tp')), parts along dimension 0
- prompt_state_out: float32 [8, 8, 128, 256], P('dp', 'tp', 'kv'), parts along dimension 0
- decode_state_out: float32 [256, 8, 128, 256], P(('dp', 'kv'), 'tp'), parts along dimension 0
The draws below stay inside these ranges and needn't reach their ends.
There are 4 independent parts, one for each index of `dp`. The reference program is written for one: setup_inputs(seed, part) draws one part's arguments, and reference() takes and returns one part's arrays. A program takes and returns all parts, laid end to end along the dimension named above; an argument that names none is the same for every part. Nothing has to cross between parts.
All inputs are finite; a program needn't handle non-finite values.
Results may differ from the reference program's by a relative error of at most 0.014.
Values may be sent and summed in bfloat16 or wider, within the bound.
A program may use at most 192 MiB of HBM per device.

```python
import jax
import jax.numpy as jnp
from jax import lax

D = 2048
HEADS = 8
DK = 128
DV = 256
BLOCK = 64
PROMPTS = 2
PIECE = 4096
DEC = 64


def block_scale(rng, extent, cuts, smallest, high):
    def one(axis_at, blocks):
        draws = jax.random.uniform(jax.random.fold_in(jax.random.fold_in(rng, 6), axis_at), (blocks,), jnp.float32, smallest / len(cuts), high / len(cuts))
        return jnp.repeat(jnp.exp(draws), extent[axis_at] // blocks).reshape((-1,) + (1,) * (len(extent) - axis_at - 1))

    level = one(*cuts[0])
    for cut in cuts[1:]:
        level = level * one(*cut)
    return level


def centred(rng, dims, spread, bound, cuts=(), held_as=jnp.bfloat16):
    values = spread * jax.random.normal(rng, dims, jnp.float32)
    if cuts:
        values = values * block_scale(rng, dims, cuts, -0.22, 0.18)
    return jnp.clip(values, -bound, bound).astype(held_as)


def setup_inputs(seed: int = 0, part: int = 0) -> dict:
    key_of = jax.random.split(jax.random.key(seed), 13)
    own_keys = jax.random.split(jax.random.fold_in(key_of[12], part), 13)
    return {
        "pieces": centred(own_keys[0], (PIECE, PROMPTS, D), 1.0, 6.0, ((0, 8),)),
        "new_tokens": centred(own_keys[1], (DEC, D), 1.0, 6.0, ((0, 8),)),
        "w_query": centred(key_of[2], (D, HEADS * DK), D ** -0.5, 0.125, ((1, 2),)),
        "w_key": centred(key_of[3], (D, HEADS * DK), D ** -0.5, 0.125, ((1, 2),)),
        "w_value": centred(key_of[4], (D, HEADS * DV), D ** -0.5, 0.125, ((1, 2),)),
        "w_decay": centred(key_of[5], (D, HEADS * DK), D ** -0.5, 0.125, ((1, 2),)),
        "decay_bias": jnp.clip(jax.random.uniform(key_of[6], (HEADS * DK,), jnp.float32, 0.0, 9.0), 0.0, 9.0),
        "norm_gain": jnp.clip(1.0 + 0.18 * jax.random.normal(key_of[7], (D,), jnp.float32), 0.1, 1.9),
        "head_gain": jnp.clip(1.0 + 0.18 * jax.random.normal(key_of[8], (HEADS * DV,), jnp.float32), 0.1, 1.9),
        "w_out": centred(key_of[9], (HEADS * DV, D), (HEADS * DV) ** -0.5, 0.125),
        "prompt_state": centred(own_keys[10], (PROMPTS, HEADS, DK, DV), 2.0, 8.0, ((1, 2), (2, 4)), jnp.float32),
        "decode_state": centred(own_keys[11], (DEC, HEADS, DK, DV), 2.0, 8.0, ((0, 4), (1, 2)), jnp.float32),
    }


highest = lax.Precision.HIGHEST
norm_eps = 0.1
decay_tau = 16.0
part_limit = 16

def rms_rows(row_block, gain):
    wide = row_block.astype(jnp.float32)
    factor = lax.rsqrt(lax.optimization_barrier(jnp.mean(wide * wide, axis=-1, keepdims=True)) + norm_eps)
    return (wide * factor * gain).astype(jnp.bfloat16)

def head_norm(outputs, gain):
    factor = lax.rsqrt(lax.optimization_barrier(jnp.mean(outputs * outputs, axis=-1, keepdims=True)) + norm_eps)
    flat = (outputs * factor).reshape(outputs.shape[:-2] + (-1,))
    return (flat * gain).astype(jnp.bfloat16)

def project_roles(row_block, w_query, w_key, w_value, w_decay, decay_bias):
    lead = row_block.shape[:-1]
    queries = (jnp.dot(row_block, w_query, preferred_element_type=jnp.float32) * DK ** (-0.5)).astype(jnp.bfloat16)
    keys_new = jnp.dot(row_block, w_key, preferred_element_type=jnp.float32).astype(jnp.bfloat16)
    values_new = jnp.dot(row_block, w_value, preferred_element_type=jnp.float32).astype(jnp.bfloat16)
    decays = jax.nn.log_sigmoid(jnp.dot(row_block, w_decay, preferred_element_type=jnp.float32) + decay_bias) / decay_tau
    return (queries.reshape(lead + (HEADS, DK)), keys_new.reshape(lead + (HEADS, DK)), values_new.reshape(lead + (HEADS, DV)), decays.reshape(lead + (HEADS, DK)))

def block_terms(q_blk, k_blk, v_blk, g_blk):
    block_len = q_blk.shape[0]
    part_len = min(part_limit, block_len)
    part_count = block_len // part_len
    within = jnp.cumsum(g_blk, axis=0)
    part_ends = within[part_len - 1::part_len]
    anchor = jnp.concatenate([jnp.zeros_like(part_ends[:1]), part_ends[:-1]], axis=0)
    q_wide = q_blk.astype(jnp.float32)
    k_wide = k_blk.astype(jnp.float32)
    q_parts = q_wide.reshape((part_count, part_len) + q_blk.shape[1:])
    w_parts = within.reshape((part_count, part_len) + within.shape[1:])
    near_query = (q_parts * jnp.exp(w_parts - anchor[:, None])).astype(jnp.bfloat16)
    near_key = (k_wide[None] * jnp.exp(anchor[:, None] - within[None])).astype(jnp.bfloat16)
    scores = jnp.einsum('itbhk,isbhk->ibhts', near_query, near_key, preferred_element_type=jnp.float32)
    row_pos = jnp.arange(part_count)[:, None] * part_len + jnp.arange(part_len)[None]
    keep = row_pos[:, :, None] >= jnp.arange(block_len)[None, None]
    weights = jnp.where(keep[:, None, None], scores, 0.0).astype(jnp.bfloat16)
    in_block = jnp.einsum('ibhts,sbhv->itbhv', weights, v_blk, preferred_element_type=jnp.float32)
    in_block = in_block.reshape((block_len,) + in_block.shape[2:])
    block_total = within[-1]
    start_query = (q_wide * jnp.exp(within)).astype(jnp.bfloat16)
    end_key = (k_wide * jnp.exp(block_total[None] - within)).astype(jnp.bfloat16)
    added = jnp.einsum('sbhk,sbhv->bhkv', end_key, v_blk, preferred_element_type=jnp.float32)
    return (in_block, start_query, block_total, added)

def block_attention(query_all, key_all, value_all, decay_all, start_states):
    seq_len = query_all.shape[0]
    block_count = seq_len // BLOCK

    def to_blocks(tensor):
        return tensor.reshape((block_count, BLOCK) + tensor.shape[1:])

    def advance(states, inputs):
        in_block, start_query, block_total, added = block_terms(*inputs)
        from_state = jnp.einsum('tbhk,bhkv->tbhv', start_query.astype(jnp.float32), states, precision=highest)
        carried = jnp.exp(block_total)[..., None] * states + added
        return (carried, from_state + in_block)
    final_states, outputs = lax.scan(advance, start_states, (to_blocks(query_all), to_blocks(key_all), to_blocks(value_all), to_blocks(decay_all)))
    return (outputs.reshape((seq_len,) + outputs.shape[2:]), final_states)

def single_token(query, key_new, value_new, decay, states):
    query = query.astype(jnp.float32)
    key_new = key_new.astype(jnp.float32)
    value_new = value_new.astype(jnp.float32)
    from_state = jnp.einsum('bhk,bhkv->bhv', query * jnp.exp(decay), states, precision=highest)
    token_score = lax.optimization_barrier(jnp.sum(query * key_new, axis=-1, keepdims=True))
    outputs = from_state + token_score * value_new
    carried = jnp.exp(decay)[..., None] * states + key_new[..., None] * value_new[..., None, :]
    return (outputs, carried)

def reference(pieces, new_tokens, w_query, w_key, w_value, w_decay, decay_bias, norm_gain, head_gain, w_out, prompt_state, decode_state):
    query_p, key_p, value_p, decay_p = project_roles(rms_rows(pieces, norm_gain), w_query, w_key, w_value, w_decay, decay_bias)
    piece_att, prompt_out = block_attention(query_p, key_p, value_p, decay_p, prompt_state)
    query_d, key_d, value_d, decay_d = project_roles(rms_rows(new_tokens, norm_gain), w_query, w_key, w_value, w_decay, decay_bias)
    decode_att, decode_out = single_token(query_d, key_d, value_d, decay_d, decode_state)
    mixed_piece = jnp.dot(head_norm(piece_att, head_gain), w_out, preferred_element_type=jnp.float32).astype(jnp.bfloat16)
    mixed_decode = jnp.dot(head_norm(decode_att, head_gain), w_out, preferred_element_type=jnp.float32).astype(jnp.bfloat16)
    return (mixed_piece, mixed_decode, prompt_out, decode_out)
```

```python
import functools

import jax
import jax.numpy as jnp
import numpy as np
from jax import lax
from jax.experimental import pallas as pl
from jax.experimental.pallas import tpu as pltpu
from jax.sharding import PartitionSpec as P

DK = 128
DV = 256
STEP = 64
PART = 16

norm_eps = 0.1
decay_tau = 16.0
f32, bf16 = jnp.float32, jnp.bfloat16
MESH = pl.DeviceIdType.MESH
PAD = 16


def dot(a, b):
    return jnp.dot(a, b, preferred_element_type=f32)


def dot_nt(a, b):
    return lax.dot_general(a, b, (((1,), (1,)), ((), ())), preferred_element_type=f32)


def dot_tn(a, b):
    return lax.dot_general(a, b, (((0,), (0,)), ((), ())), preferred_element_type=f32)


def sum_matrices(prompts):
    n = STEP * prompts
    r, c = np.arange(n)[:, None], np.arange(n)[None]
    same = (r % prompts) == (c % prompts)

    def from_anchor(edge):
        return (same & (c >= edge) & (c <= r)) * 1.0 - (same & (c < edge) & (c > r)) * 1.0

    b = (same & (c <= r)) * 1.0
    rest = (same & (c > r)) * 1.0
    d0 = from_anchor(PART * prompts)[: n // 2]
    d1 = from_anchor(3 * PART * prompts)
    one = np.concatenate([b, rest, d0, d1], axis=0)
    return np.concatenate([one, one, one], axis=1)


def meet_partner(other):
    barrier = pltpu.get_barrier_semaphore()
    pl.semaphore_signal(barrier, inc=1, device_id={"tp": other}, device_id_type=MESH)
    pl.semaphore_wait(barrier, 1)


def front_kernel(
    own, chunk, prompts, heads,
    x_hbm, dec_ref, wq_hbm, wk_hbm, wv_hbm, wd_hbm, bias_ref, gain_ref, mats_ref,
    out_ref, qt_ref, st_ref, tot_ref, dp_ref,
    xb, nb, nd, wq, wk, wv, wd, qs, ks, vs, gs,
    x_sem, w_sem, send_sem, recv_sem, dsend, drecv,
):
    me = lax.axis_index("tp")
    other = 1 - me
    count = own // chunk
    for j in range(count):
        pltpu.make_async_copy(x_hbm.at[pl.ds(j * chunk, chunk)], xb.at[pl.ds(j * chunk, chunk)], x_sem.at[j]).start()
    loads = [
        pltpu.make_async_copy(src, dst, w_sem.at[i])
        for i, (src, dst) in enumerate(((wq_hbm, wq), (wk_hbm, wk), (wv_hbm, wv), (wd_hbm, wd)))
    ]
    for load in loads:
        load.start()
    meet_partner(other)

    def normed(rows):
        wide = rows.astype(f32)
        factor = lax.rsqrt(jnp.mean(wide * wide, axis=-1, keepdims=True) + norm_eps)
        return (wide * factor * gain_ref[...]).astype(bf16)

    def piece_copy(j):
        rows = pl.ds(pl.multiple_of(me * own + j * chunk, chunk), chunk)
        return pltpu.make_async_remote_copy(
            src_ref=nb.at[rows], dst_ref=nb.at[rows], send_sem=send_sem.at[j], recv_sem=recv_sem.at[j],
            device_id={"tp": other}, device_id_type=MESH,
        )

    mine = pl.ds(pl.multiple_of(me * PAD, PAD), PAD)
    nd[mine, :] = normed(dec_ref[...])
    dec_copy = pltpu.make_async_remote_copy(
        src_ref=nd.at[mine], dst_ref=nd.at[mine], send_sem=dsend, recv_sem=drecv,
        device_id={"tp": other}, device_id_type=MESH,
    )
    small = min(64, chunk)
    for j in range(count):
        pltpu.make_async_copy(x_hbm.at[pl.ds(j * chunk, chunk)], xb.at[pl.ds(j * chunk, chunk)], x_sem.at[j]).wait()

        @pl.loop(0, chunk // small)
        def _(s):
            at = j * chunk + s * small
            nb[pl.ds(pl.multiple_of(me * own + at, small), small), :] = normed(xb[pl.ds(pl.multiple_of(at, small), small), :])

        if j == 0:
            dec_copy.start()
        else:
            piece_copy(j - 1).start()
    piece_copy(count - 1).start()
    for load in loads:
        load.wait()

    def decay_of(product):
        t = product + bias_ref[...]
        return (jnp.minimum(t, 0.0) - jnp.log1p(jnp.exp(-jnp.abs(t)))) * (1.0 / decay_tau)

    def project(at):
        rows = pl.ds(pl.multiple_of(at, chunk), chunk)
        block = nb[rows, :]
        qs[rows, :] = (dot(block, wq[...]) * DK ** (-0.5)).astype(bf16)
        ks[rows, :] = dot(block, wk[...]).astype(bf16)
        half = wv.shape[1] // 2
        vs[rows, :half] = dot(block, wv[:, :half]).astype(bf16)
        vs[rows, half:] = dot(block, wv[:, half:]).astype(bf16)
        gs[rows, :] = decay_of(dot(block, wd[...]))

    @pl.loop(0, count)
    def _(j):
        project(me * own + j * chunk)

    @pl.loop(0, count)
    def _(j):
        rows = pl.ds(pl.multiple_of(other * own + j * chunk, chunk), chunk)
        pltpu.make_async_remote_copy(
            src_ref=nb.at[rows], dst_ref=nb.at[rows], send_sem=send_sem.at[j], recv_sem=recv_sem.at[j],
            device_id={"tp": other}, device_id_type=MESH,
        ).wait_recv()
        project(other * own + j * chunk)

    for j in range(count):
        piece_copy(j).wait_send()
    dec_copy.wait()
    dec_rows = nd[...]
    qk = wq.shape[1]
    dp_ref[:, :qk] = (dot(dec_rows, wq[...]) * DK ** (-0.5)).astype(bf16).astype(f32)
    dp_ref[:, qk : 2 * qk] = dot(dec_rows, wk[...]).astype(bf16).astype(f32)
    dp_ref[:, 2 * qk : 3 * qk] = decay_of(dot(dec_rows, wd[...]))
    dp_ref[:, 3 * qk :] = dot(dec_rows, wv[...]).astype(bf16).astype(f32)

    n = STEP * prompts
    half = n // 2
    st_ref[...] = jnp.zeros_like(st_ref)
    tot_ref[...] = jnp.zeros_like(tot_ref)

    @pl.loop(0, 2 * own // n)
    def _(i):
        rows = pl.ds(pl.multiple_of(i * n, n), n)
        g = gs[rows, :]
        hi = g.astype(bf16)
        left = g - hi.astype(f32)
        mid = left.astype(bf16)
        low = (left - mid.astype(f32)).astype(bf16)
        sums = dot(mats_ref[...], jnp.concatenate([hi, mid, low], axis=0))
        b, rest = sums[:n], sums[n : 2 * n]
        d0, d1 = sums[2 * n : 2 * n + half], sums[2 * n + half :]
        q = qs[rows, :].astype(f32)
        k = ks[rows, :].astype(f32)
        row_prompt = lax.broadcasted_iota(jnp.int32, (n, 1), 0) % prompts
        offset = tot_ref[0:1, :]
        for p in range(1, prompts):
            offset = jnp.where(row_prompt == p, tot_ref[p : p + 1, :], offset)
        qt_ref[rows, :] = (q * jnp.exp(b + offset)).astype(bf16)
        start_query = (q * jnp.exp(b)).astype(bf16)
        end_key = (k * jnp.exp(rest)).astype(bf16)
        near_q0 = (q[:half] * jnp.exp(d0)).astype(bf16)
        near_k0 = (k[:half] * jnp.exp(-d0)).astype(bf16)
        near_q1 = (q[half:] * jnp.exp(d1[half:])).astype(bf16)
        near_k1 = (k * jnp.exp(-d1)).astype(bf16)
        block_total = b[n - prompts :]
        decay = jnp.exp(block_total)
        tot_ref[:prompts, :] = tot_ref[:prompts, :] + block_total
        r_at = lax.broadcasted_iota(jnp.int32, (n, n), 0)
        c_at = lax.broadcasted_iota(jnp.int32, (n, n), 1)
        keep = (c_at <= r_at) & (r_at % prompts == c_at % prompts)
        for h in range(heads):
            kc = slice(h * DK, (h + 1) * DK)
            v = vs[rows, h * DV : (h + 1) * DV]
            w0 = jnp.where(keep[:half, :half], dot_nt(near_q0[:, kc], near_k0[:, kc]), 0.0).astype(bf16)
            w1 = jnp.where(keep[half:], dot_nt(near_q1[:, kc], near_k1[:, kc]), 0.0).astype(bf16)
            inner = jnp.concatenate([dot(w0, v[:half]), dot(w1, v)], axis=0)
            state = st_ref[h]
            from_all = dot_nt(start_query[:, kc], state.astype(bf16))
            from_state = from_all[:, :DV]
            for p in range(1, prompts):
                from_state = jnp.where(row_prompt == p, from_all[:, p * DV : (p + 1) * DV], from_state)
            out_ref[rows, h * DV : (h + 1) * DV] = (inner + from_state).astype(bf16)
            zero = jnp.zeros_like(v)
            v_each = jnp.concatenate([jnp.where(row_prompt == p, v, zero) for p in range(prompts)], axis=1)
            added = dot_tn(v_each, end_key[:, kc])
            for p in range(prompts):
                at = slice(p * DV, (p + 1) * DV)
                st_ref[h, at, :] = state[at] * decay[p : p + 1, kc] + added[at]


def back_kernel(
    own, chunk, prompts, heads,
    out_ref, qt_ref, in_ref, gain_ref, dec_ref, w_hbm,
    y_ref, yd_ref,
    w, nl, nr, dl, dr,
    w_sem, send_sem, recv_sem, dsend, drecv,
):
    me = lax.axis_index("tp")
    other = 1 - me
    count = own // chunk
    load = pltpu.make_async_copy(w_hbm, w, w_sem)
    load.start()
    meet_partner(other)

    def head_norm(part, h):
        factor = lax.rsqrt(jnp.mean(part * part, axis=-1, keepdims=True) + norm_eps)
        return (part * factor * gain_ref[:, h * DV : (h + 1) * DV]).astype(bf16)

    def finish(at):
        rows = pl.ds(pl.multiple_of(at, chunk), chunk)
        row_prompt = lax.broadcasted_iota(jnp.int32, (chunk, 1), 0) % prompts
        for h in range(heads):
            cols = slice(h * DV, (h + 1) * DV)
            from_all = dot_nt(qt_ref[rows, h * DK : (h + 1) * DK], in_ref[h])
            from_state = from_all[:, :DV]
            for p in range(1, prompts):
                from_state = jnp.where(row_prompt == p, from_all[:, p * DV : (p + 1) * DV], from_state)
            nl[rows, cols] = head_norm(out_ref[rows, cols].astype(f32) + from_state, h)

    def copy(j):
        src = pl.ds(pl.multiple_of(other * own + j * chunk, chunk), chunk)
        return pltpu.make_async_remote_copy(
            src_ref=nl.at[src], dst_ref=nr.at[pl.ds(j * chunk, chunk)], send_sem=send_sem.at[j], recv_sem=recv_sem.at[j],
            device_id={"tp": other}, device_id_type=MESH,
        )

    for h in range(heads):
        cols = slice(h * DV, (h + 1) * DV)
        dl[:, cols] = head_norm(dec_ref[:, cols], h)
    dec_copy = pltpu.make_async_remote_copy(
        src_ref=dl.at[pl.ds(pl.multiple_of(other * PAD, PAD), PAD)], dst_ref=dr, send_sem=dsend, recv_sem=drecv,
        device_id={"tp": other}, device_id_type=MESH,
    )
    for j in range(count):
        finish(other * own + j * chunk)
        if j == 0:
            dec_copy.start()
        else:
            copy(j - 1).start()
    finish(me * own)
    copy(count - 1).start()

    if count > 1:
        @pl.loop(1, count)
        def _(j):
            finish(me * own + j * chunk)

    load.wait()
    width = nl.shape[1]
    w_mine = pl.ds(pl.multiple_of(me * width, width), width)
    w_other = pl.ds(pl.multiple_of(other * width, width), width)
    tile = 512
    for j in range(count):
        copy(j).wait_recv()

        @pl.loop(0, w.shape[1] // tile)
        def _(t):
            cols = pl.ds(pl.multiple_of(t * tile, tile), tile)
            held = nl[pl.ds(pl.multiple_of(me * own + j * chunk, chunk), chunk), :]
            y_ref[pl.ds(j * chunk, chunk), cols] = (
                dot(held, w[w_mine, cols]) + dot(nr[pl.ds(j * chunk, chunk), :], w[w_other, cols])
            ).astype(bf16)

    dec_copy.wait()
    held = dl[pl.ds(pl.multiple_of(me * PAD, PAD), PAD), :]
    yd_ref[...] = (dot(held, w[w_mine, :]) + dot(dr[...], w[w_other, :])).astype(bf16)
    for j in range(count):
        copy(j).wait_send()


def decode_kernel(heads, cols_ref, v_ref, s_ref, att_ref, new_ref):
    for h in range(heads):
        state = s_ref[0, h]
        qe = cols_ref[0, :, h : h + 1]
        e = cols_ref[0, :, heads + h : heads + h + 1]
        k = cols_ref[0, :, 2 * heads + h : 2 * heads + h + 1]
        qk = cols_ref[0, 0:1, 3 * heads + h : 3 * heads + h + 1]
        v = v_ref[0, :, h * DV : (h + 1) * DV]
        att_ref[0, :, h * DV : (h + 1) * DV] = jnp.sum(qe * state, axis=0, keepdims=True) + qk * v
        new_ref[0, h] = e * state + k * v


ANY = pl.BlockSpec(memory_space=pl.ANY)
VMEM = pl.BlockSpec(memory_space=pltpu.VMEM)
LIMIT = 60 * 1024 * 1024


def on_device(
    pieces, new_tokens, w_query, w_key, w_value, w_decay, decay_bias, norm_gain, head_gain, w_out, prompt_state, decode_state,
):
    kv_size = lax.axis_size("kv")
    tp_index = lax.axis_index("tp")
    kv_index = lax.axis_index("kv")
    qk = w_query.shape[1]
    heads = qk // DK
    vw = heads * DV
    own_pos, prompts, width = pieces.shape
    own = own_pos * prompts
    chunk = min(256, own)
    count = own // chunk
    rows = 2 * own
    dec_own = new_tokens.shape[0]
    bias_here = lax.dynamic_slice_in_dim(decay_bias, tp_index * qk, qk)[None]
    gain_here = lax.dynamic_slice_in_dim(head_gain, tp_index * vw, vw)[None]
    whole_start = lax.all_gather(prompt_state.astype(bf16), "kv", axis=2, tiled=True)
    whole_start = whole_start.transpose(1, 0, 3, 2).astype(f32)

    mats = jnp.asarray(sum_matrices(prompts), bf16)
    dec_rows = jnp.pad(new_tokens, ((0, PAD - dec_own), (0, 0)))
    proj_flops = 2 * rows * width * (3 * qk + vw)
    out_local, q_total, local, totals, dec_prod = pl.pallas_call(
        functools.partial(front_kernel, own, chunk, prompts, heads),
        name="front",
        out_shape=(
            jax.ShapeDtypeStruct((rows, vw), bf16),
            jax.ShapeDtypeStruct((rows, qk), bf16),
            jax.ShapeDtypeStruct((heads, prompts * DV, DK), f32),
            jax.ShapeDtypeStruct((8, qk), f32),
            jax.ShapeDtypeStruct((2 * PAD, 3 * qk + vw), f32),
        ),
        in_specs=[ANY, VMEM, ANY, ANY, ANY, ANY, VMEM, VMEM, VMEM],
        out_specs=(VMEM,) * 5,
        scratch_shapes=[
            pltpu.VMEM((own, width), bf16),
            pltpu.VMEM((rows, width), bf16),
            pltpu.VMEM((2 * PAD, width), bf16),
            pltpu.VMEM((width, qk), bf16),
            pltpu.VMEM((width, qk), bf16),
            pltpu.VMEM((width, vw), bf16),
            pltpu.VMEM((width, qk), bf16),
            pltpu.VMEM((rows, qk), bf16),
            pltpu.VMEM((rows, qk), bf16),
            pltpu.VMEM((rows, vw), bf16),
            pltpu.VMEM((rows, qk), f32),
            pltpu.SemaphoreType.DMA((count,)),
            pltpu.SemaphoreType.DMA((4,)),
            pltpu.SemaphoreType.DMA((count,)),
            pltpu.SemaphoreType.DMA((count,)),
            pltpu.SemaphoreType.DMA,
            pltpu.SemaphoreType.DMA,
        ],
        compiler_params=pltpu.CompilerParams(collective_id=0, has_side_effects=True, vmem_limit_bytes=LIMIT),
        cost_estimate=pl.CostEstimate(flops=proj_flops, bytes_accessed=20_000_000, transcendentals=0),
    )(pieces.reshape(own, width), dec_rows, w_query, w_key, w_value, w_decay, bias_here, norm_gain[None], mats)

    totals = totals[:prompts].reshape(prompts, heads, DK).transpose(1, 0, 2)[:, :, None]
    local = local.reshape(heads, prompts, DV, DK)
    all_local = lax.all_gather(local.astype(bf16), "kv")
    all_totals = lax.all_gather(totals, "kv")

    dec_all = dec_prod.reshape(2, PAD, -1)[:, :dec_own].reshape(2 * dec_own, -1)
    seqs = 2 * dec_own
    q_d = dec_all[:, :qk].reshape(seqs, heads, DK)
    k_d = dec_all[:, qk : 2 * qk].reshape(seqs, heads, DK)
    e_d = jnp.exp(dec_all[:, 2 * qk : 3 * qk]).reshape(seqs, heads, DK)
    qk_d = jnp.broadcast_to(jnp.sum(q_d * k_d, axis=-1, keepdims=True), q_d.shape)
    cols = jnp.concatenate([q_d * e_d, e_d, k_d, qk_d], axis=1).transpose(0, 2, 1)
    v_d = dec_all[:, 3 * qk :][:, None]
    dec_att, decode_out = pl.pallas_call(
        functools.partial(decode_kernel, heads),
        name="decode",
        grid=(seqs,),
        out_shape=(
            jax.ShapeDtypeStruct((seqs, 1, vw), f32),
            jax.ShapeDtypeStruct(decode_state.shape, f32),
        ),
        in_specs=[
            pl.BlockSpec((1, DK, 4 * heads), lambda i: (i, 0, 0)),
            pl.BlockSpec((1, 1, vw), lambda i: (i, 0, 0)),
            pl.BlockSpec((1, heads, DK, DV), lambda i: (i, 0, 0, 0)),
        ],
        out_specs=(
            pl.BlockSpec((1, 1, vw), lambda i: (i, 0, 0)),
            pl.BlockSpec((1, heads, DK, DV), lambda i: (i, 0, 0, 0)),
        ),
        cost_estimate=pl.CostEstimate(flops=8 * decode_state.size, bytes_accessed=8 * decode_state.size, transcendentals=0),
    )(cols, v_d, decode_state)

    running = whole_start
    incoming = whole_start
    for c in range(kv_size):
        incoming = jnp.where(kv_index == c, running, incoming)
        running = jnp.exp(all_totals[c]) * running + all_local[c].astype(f32)
    rows_k = prompt_state.shape[2]
    prompt_out = lax.dynamic_slice_in_dim(running, kv_index * rows_k, rows_k, 3).transpose(1, 0, 3, 2)

    dec_pad = jnp.pad(dec_att.reshape(2, dec_own, vw), ((0, 0), (0, PAD - dec_own), (0, 0))).reshape(2 * PAD, vw)
    y, yd = pl.pallas_call(
        functools.partial(back_kernel, own, chunk, prompts, heads),
        name="back",
        out_shape=(
            jax.ShapeDtypeStruct((own, w_out.shape[1]), bf16),
            jax.ShapeDtypeStruct((PAD, w_out.shape[1]), bf16),
        ),
        in_specs=[VMEM] * 5 + [ANY],
        out_specs=(VMEM,) * 2,
        scratch_shapes=[
            pltpu.VMEM(w_out.shape, bf16),
            pltpu.VMEM((rows, vw), bf16),
            pltpu.VMEM((own, vw), bf16),
            pltpu.VMEM((2 * PAD, vw), bf16),
            pltpu.VMEM((PAD, vw), bf16),
            pltpu.SemaphoreType.DMA,
            pltpu.SemaphoreType.DMA((count,)),
            pltpu.SemaphoreType.DMA((count,)),
            pltpu.SemaphoreType.DMA,
            pltpu.SemaphoreType.DMA,
        ],
        compiler_params=pltpu.CompilerParams(collective_id=1, has_side_effects=True, vmem_limit_bytes=LIMIT),
        cost_estimate=pl.CostEstimate(flops=2 * own * w_out.size, bytes_accessed=20_000_000, transcendentals=0),
    )(out_local, q_total, incoming.reshape(heads, prompts * DV, DK).astype(bf16), gain_here, dec_pad, w_out)
    return (y.reshape(own_pos, prompts, -1), yd[:dec_own], prompt_out, decode_out)


def solution(mesh):
    return jax.shard_map(
        on_device,
        mesh=mesh,
        in_specs=(
            P(("kv", "tp"), "dp", None),
            P(("dp", "kv", "tp"), None),
            P(None, "tp"),
            P(None, "tp"),
            P(None, "tp"),
            P(None, "tp"),
            P(),
            P(),
            P(),
            P(),
            P("dp", "tp", "kv", None),
            P(("dp", "kv"), "tp", None, None),
        ),
        out_specs=(
            P(("kv", "tp"), "dp", None),
            P(("dp", "kv", "tp"), None),
            P("dp", "tp", "kv", None),
            P(("dp", "kv"), "tp", None, None),
        ),
        check_vma=False,
    )
```

```python
import functools

import jax
import jax.numpy as jnp
import numpy as np
from jax import lax
from jax.experimental import pallas as pl
from jax.experimental.pallas import tpu as pltpu
from jax.sharding import PartitionSpec as P

DK = 128
DV = 256
STEP = 64
PART = 16

norm_eps = 0.1
decay_tau = 16.0
f32, bf16 = jnp.float32, jnp.bfloat16
MESH = pl.DeviceIdType.MESH
PAD = 16


def dot(a, b):
    return jnp.dot(a, b, preferred_element_type=f32)


def dot_nt(a, b):
    return lax.dot_general(a, b, (((1,), (1,)), ((), ())), preferred_element_type=f32)


def dot_tn(a, b):
    return lax.dot_general(a, b, (((0,), (0,)), ((), ())), preferred_element_type=f32)


def sum_matrices(prompts):
    n = STEP * prompts
    r, c = np.arange(n)[:, None], np.arange(n)[None]
    same = (r % prompts) == (c % prompts)

    def from_anchor(edge):
        return (same & (c >= edge) & (c <= r)) * 1.0 - (same & (c < edge) & (c > r)) * 1.0

    b = (same & (c <= r)) * 1.0
    rest = (same & (c > r)) * 1.0
    d0 = from_anchor(PART * prompts)[: n // 2]
    d1 = from_anchor(3 * PART * prompts)
    one = np.concatenate([b, rest, d0, d1], axis=0)
    return np.concatenate([one, one, one], axis=1)


def meet_partner(other):
    barrier = pltpu.get_barrier_semaphore()
    pl.semaphore_signal(barrier, inc=1, device_id={"tp": other}, device_id_type=MESH)
    pl.semaphore_wait(barrier, 1)


def front_kernel(
    own, chunk, prompts, heads,
    x_hbm, dec_ref, wq_hbm, wk_hbm, wv_hbm, wd_hbm, bias_ref, gain_ref, mats_ref,
    out_ref, qt_ref, st_ref, tot_ref, dp_ref,
    xb, nb, nd, wq, wk, wv, wd, qs, ks, vs, gs,
    x_sem, w_sem, send_sem, recv_sem, dsend, drecv,
):
    me = lax.axis_index("tp")
    other = 1 - me
    count = own // chunk
    for j in range(count):
        pltpu.make_async_copy(x_hbm.at[pl.ds(j * chunk, chunk)], xb.at[pl.ds(j * chunk, chunk)], x_sem.at[j]).start()
    loads = [
        pltpu.make_async_copy(src, dst, w_sem.at[i])
        for i, (src, dst) in enumerate(((wq_hbm, wq), (wk_hbm, wk), (wv_hbm, wv), (wd_hbm, wd)))
    ]
    for load in loads:
        load.start()
    meet_partner(other)

    def normed(rows):
        wide = rows.astype(f32)
        factor = lax.rsqrt(jnp.mean(wide * wide, axis=-1, keepdims=True) + norm_eps)
        return (wide * factor * gain_ref[...]).astype(bf16)

    def piece_copy(j):
        rows = pl.ds(pl.multiple_of(me * own + j * chunk, chunk), chunk)
        return pltpu.make_async_remote_copy(
            src_ref=nb.at[rows], dst_ref=nb.at[rows], send_sem=send_sem.at[j], recv_sem=recv_sem.at[j],
            device_id={"tp": other}, device_id_type=MESH,
        )

    mine = pl.ds(pl.multiple_of(me * PAD, PAD), PAD)
    nd[mine, :] = normed(dec_ref[...])
    dec_copy = pltpu.make_async_remote_copy(
        src_ref=nd.at[mine], dst_ref=nd.at[mine], send_sem=dsend, recv_sem=drecv,
        device_id={"tp": other}, device_id_type=MESH,
    )
    small = min(64, chunk)
    for j in range(count):
        pltpu.make_async_copy(x_hbm.at[pl.ds(j * chunk, chunk)], xb.at[pl.ds(j * chunk, chunk)], x_sem.at[j]).wait()

        @pl.loop(0, chunk // small)
        def _(s):
            at = j * chunk + s * small
            nb[pl.ds(pl.multiple_of(me * own + at, small), small), :] = normed(xb[pl.ds(pl.multiple_of(at, small), small), :])

        if j == 0:
            dec_copy.start()
        else:
            piece_copy(j - 1).start()
    piece_copy(count - 1).start()
    for load in loads:
        load.wait()

    def decay_of(product):
        t = product + bias_ref[...]
        return (jnp.minimum(t, 0.0) - jnp.log1p(jnp.exp(-jnp.abs(t)))) * (1.0 / decay_tau)

    def project(at):
        rows = pl.ds(pl.multiple_of(at, chunk), chunk)
        block = nb[rows, :]
        qs[rows, :] = (dot(block, wq[...]) * DK ** (-0.5)).astype(bf16)
        ks[rows, :] = dot(block, wk[...]).astype(bf16)
        half = wv.shape[1] // 2
        vs[rows, :half] = dot(block, wv[:, :half]).astype(bf16)
        vs[rows, half:] = dot(block, wv[:, half:]).astype(bf16)
        gs[rows, :] = decay_of(dot(block, wd[...]))

    @pl.loop(0, count)
    def _(j):
        project(me * own + j * chunk)

    @pl.loop(0, count)
    def _(j):
        rows = pl.ds(pl.multiple_of(other * own + j * chunk, chunk), chunk)
        pltpu.make_async_remote_copy(
            src_ref=nb.at[rows], dst_ref=nb.at[rows], send_sem=send_sem.at[j], recv_sem=recv_sem.at[j],
            device_id={"tp": other}, device_id_type=MESH,
        ).wait_recv()
        project(other * own + j * chunk)

    for j in range(count):
        piece_copy(j).wait_send()
    dec_copy.wait()
    dec_rows = nd[...]
    qk = wq.shape[1]
    dp_ref[:, :qk] = (dot(dec_rows, wq[...]) * DK ** (-0.5)).astype(bf16).astype(f32)
    dp_ref[:, qk : 2 * qk] = dot(dec_rows, wk[...]).astype(bf16).astype(f32)
    dp_ref[:, 2 * qk : 3 * qk] = decay_of(dot(dec_rows, wd[...]))
    dp_ref[:, 3 * qk :] = dot(dec_rows, wv[...]).astype(bf16).astype(f32)

    n = STEP * prompts
    half = n // 2
    st_ref[...] = jnp.zeros_like(st_ref)
    tot_ref[...] = jnp.zeros_like(tot_ref)

    @pl.loop(0, 2 * own // n)
    def _(i):
        rows = pl.ds(pl.multiple_of(i * n, n), n)
        g = gs[rows, :]
        hi = g.astype(bf16)
        left = g - hi.astype(f32)
        mid = left.astype(bf16)
        low = (left - mid.astype(f32)).astype(bf16)
        sums = dot(mats_ref[...], jnp.concatenate([hi, mid, low], axis=0))
        b, rest = sums[:n], sums[n : 2 * n]
        d0, d1 = sums[2 * n : 2 * n + half], sums[2 * n + half :]
        q = qs[rows, :].astype(f32)
        k = ks[rows, :].astype(f32)
        row_prompt = lax.broadcasted_iota(jnp.int32, (n, 1), 0) % prompts
        offset = tot_ref[0:1, :]
        for p in range(1, prompts):
            offset = jnp.where(row_prompt == p, tot_ref[p : p + 1, :], offset)
        qt_ref[rows, :] = (q * jnp.exp(b + offset)).astype(bf16)
        start_query = (q * jnp.exp(b)).astype(bf16)
        end_key = (k * jnp.exp(rest)).astype(bf16)
        near_q0 = (q[:half] * jnp.exp(d0)).astype(bf16)
        near_k0 = (k[:half] * jnp.exp(-d0)).astype(bf16)
        near_q1 = (q[half:] * jnp.exp(d1[half:])).astype(bf16)
        near_k1 = (k * jnp.exp(-d1)).astype(bf16)
        block_total = b[n - prompts :]
        decay = jnp.exp(block_total)
        tot_ref[:prompts, :] = tot_ref[:prompts, :] + block_total
        r_at = lax.broadcasted_iota(jnp.int32, (n, n), 0)
        c_at = lax.broadcasted_iota(jnp.int32, (n, n), 1)
        keep = (c_at <= r_at) & (r_at % prompts == c_at % prompts)
        for h in range(heads):
            kc = slice(h * DK, (h + 1) * DK)
            v = vs[rows, h * DV : (h + 1) * DV]
            w0 = jnp.where(keep[:half, :half], dot_nt(near_q0[:, kc], near_k0[:, kc]), 0.0).astype(bf16)
            w1 = jnp.where(keep[half:], dot_nt(near_q1[:, kc], near_k1[:, kc]), 0.0).astype(bf16)
            inner = jnp.concatenate([dot(w0, v[:half]), dot(w1, v)], axis=0)
            state = st_ref[h]
            from_all = dot_nt(start_query[:, kc], state.astype(bf16))
            from_state = from_all[:, :DV]
            for p in range(1, prompts):
                from_state = jnp.where(row_prompt == p, from_all[:, p * DV : (p + 1) * DV], from_state)
            out_ref[rows, h * DV : (h + 1) * DV] = (inner + from_state).astype(bf16)
            zero = jnp.zeros_like(v)
            v_each = jnp.concatenate([jnp.where(row_prompt == p, v, zero) for p in range(prompts)], axis=1)
            added = dot_tn(v_each, end_key[:, kc])
            for p in range(prompts):
                at = slice(p * DV, (p + 1) * DV)
                st_ref[h, at, :] = state[at] * decay[p : p + 1, kc] + added[at]


def back_kernel(
    own, chunk, prompts, heads,
    out_ref, qt_ref, in_ref, gain_ref, dec_ref, w_hbm,
    y_ref, yd_ref,
    w, nl, nr, dl, dr,
    w_sem, send_sem, recv_sem, dsend, drecv,
):
    me = lax.axis_index("tp")
    other = 1 - me
    count = own // chunk
    load = pltpu.make_async_copy(w_hbm, w, w_sem)
    load.start()
    meet_partner(other)

    def head_norm(part, h):
        factor = lax.rsqrt(jnp.mean(part * part, axis=-1, keepdims=True) + norm_eps)
        return (part * factor * gain_ref[:, h * DV : (h + 1) * DV]).astype(bf16)

    def finish(at):
        rows = pl.ds(pl.multiple_of(at, chunk), chunk)
        row_prompt = lax.broadcasted_iota(jnp.int32, (chunk, 1), 0) % prompts
        for h in range(heads):
            cols = slice(h * DV, (h + 1) * DV)
            from_all = dot_nt(qt_ref[rows, h * DK : (h + 1) * DK], in_ref[h])
            from_state = from_all[:, :DV]
            for p in range(1, prompts):
                from_state = jnp.where(row_prompt == p, from_all[:, p * DV : (p + 1) * DV], from_state)
            nl[rows, cols] = head_norm(out_ref[rows, cols].astype(f32) + from_state, h)

    def copy(j):
        src = pl.ds(pl.multiple_of(other * own + j * chunk, chunk), chunk)
        return pltpu.make_async_remote_copy(
            src_ref=nl.at[src], dst_ref=nr.at[pl.ds(j * chunk, chunk)], send_sem=send_sem.at[j], recv_sem=recv_sem.at[j],
            device_id={"tp": other}, device_id_type=MESH,
        )

    for h in range(heads):
        cols = slice(h * DV, (h + 1) * DV)
        dl[:, cols] = head_norm(dec_ref[:, cols], h)
    dec_copy = pltpu.make_async_remote_copy(
        src_ref=dl.at[pl.ds(pl.multiple_of(other * PAD, PAD), PAD)], dst_ref=dr, send_sem=dsend, recv_sem=drecv,
        device_id={"tp": other}, device_id_type=MESH,
    )
    for j in range(count):
        finish(other * own + j * chunk)
        if j == 0:
            dec_copy.start()
        else:
            copy(j - 1).start()
    finish(me * own)
    copy(count - 1).start()

    if count > 1:
        @pl.loop(1, count)
        def _(j):
            finish(me * own + j * chunk)

    load.wait()
    width = nl.shape[1]
    w_mine = pl.ds(pl.multiple_of(me * width, width), width)
    w_other = pl.ds(pl.multiple_of(other * width, width), width)
    tile = 512
    for j in range(count):
        copy(j).wait_recv()

        @pl.loop(0, w.shape[1] // tile)
        def _(t):
            cols = pl.ds(pl.multiple_of(t * tile, tile), tile)
            held = nl[pl.ds(pl.multiple_of(me * own + j * chunk, chunk), chunk), :]
            y_ref[pl.ds(j * chunk, chunk), cols] = (
                dot(held, w[w_mine, cols]) + dot(nr[pl.ds(j * chunk, chunk), :], w[w_other, cols])
            ).astype(bf16)

    dec_copy.wait()
    held = dl[pl.ds(pl.multiple_of(me * PAD, PAD), PAD), :]
    yd_ref[...] = (dot(held, w[w_mine, :]) + dot(dr[...], w[w_other, :])).astype(bf16)
    for j in range(count):
        copy(j).wait_send()


def decode_kernel(heads, cols_ref, v_ref, s_ref, att_ref, new_ref):
    for h in range(heads):
        state = s_ref[0, h]
        qe = cols_ref[0, :, h : h + 1]
        e = cols_ref[0, :, heads + h : heads + h + 1]
        k = cols_ref[0, :, 2 * heads + h : 2 * heads + h + 1]
        qk = cols_ref[0, 0:1, 3 * heads + h : 3 * heads + h + 1]
        v = v_ref[0, :, h * DV : (h + 1) * DV]
        att_ref[0, :, h * DV : (h + 1) * DV] = jnp.sum(qe * state, axis=0, keepdims=True) + qk * v
        new_ref[0, h] = e * state + k * v


ANY = pl.BlockSpec(memory_space=pl.ANY)
VMEM = pl.BlockSpec(memory_space=pltpu.VMEM)
LIMIT = 60 * 1024 * 1024


def on_device(
    pieces, new_tokens, w_query, w_key, w_value, w_decay, decay_bias, norm_gain, head_gain, w_out, prompt_state, decode_state,
):
    kv_size = lax.axis_size("kv")
    tp_index = lax.axis_index("tp")
    kv_index = lax.axis_index("kv")
    qk = w_query.shape[1]
    heads = qk // DK
    vw = heads * DV
    own_pos, prompts, width = pieces.shape
    own = own_pos * prompts
    chunk = min(256, own)
    count = own // chunk
    rows = 2 * own
    dec_own = new_tokens.shape[0]
    bias_here = lax.dynamic_slice_in_dim(decay_bias, tp_index * qk, qk)[None]
    gain_here = lax.dynamic_slice_in_dim(head_gain, tp_index * vw, vw)[None]
    rows_k = prompt_state.shape[2]
    start_here = prompt_state.astype(bf16).transpose(1, 0, 2, 3).reshape(heads, -1, DK)

    mats = jnp.asarray(sum_matrices(prompts), bf16)
    dec_rows = jnp.pad(new_tokens, ((0, PAD - dec_own), (0, 0)))
    proj_flops = 2 * rows * width * (3 * qk + vw)
    out_local, q_total, local, totals, dec_prod = pl.pallas_call(
        functools.partial(front_kernel, own, chunk, prompts, heads),
        name="front",
        out_shape=(
            jax.ShapeDtypeStruct((rows, vw), bf16),
            jax.ShapeDtypeStruct((rows, qk), bf16),
            jax.ShapeDtypeStruct((heads, prompts * DV, DK), f32),
            jax.ShapeDtypeStruct((8, qk), f32),
            jax.ShapeDtypeStruct((2 * PAD, 3 * qk + vw), f32),
        ),
        in_specs=[ANY, VMEM, ANY, ANY, ANY, ANY, VMEM, VMEM, VMEM],
        out_specs=(VMEM,) * 5,
        scratch_shapes=[
            pltpu.VMEM((own, width), bf16),
            pltpu.VMEM((rows, width), bf16),
            pltpu.VMEM((2 * PAD, width), bf16),
            pltpu.VMEM((width, qk), bf16),
            pltpu.VMEM((width, qk), bf16),
            pltpu.VMEM((width, vw), bf16),
            pltpu.VMEM((width, qk), bf16),
            pltpu.VMEM((rows, qk), bf16),
            pltpu.VMEM((rows, qk), bf16),
            pltpu.VMEM((rows, vw), bf16),
            pltpu.VMEM((rows, qk), f32),
            pltpu.SemaphoreType.DMA((count,)),
            pltpu.SemaphoreType.DMA((4,)),
            pltpu.SemaphoreType.DMA((count,)),
            pltpu.SemaphoreType.DMA((count,)),
            pltpu.SemaphoreType.DMA,
            pltpu.SemaphoreType.DMA,
        ],
        compiler_params=pltpu.CompilerParams(collective_id=0, has_side_effects=True, vmem_limit_bytes=LIMIT),
        cost_estimate=pl.CostEstimate(flops=proj_flops, bytes_accessed=20_000_000, transcendentals=0),
    )(pieces.reshape(own, width), dec_rows, w_query, w_key, w_value, w_decay, bias_here, norm_gain[None], mats)

    totals = totals[:prompts].reshape(prompts, heads, DK).transpose(1, 0, 2)[:, :, None]
    local = local.reshape(heads, prompts, DV, DK)
    flat_totals = totals[:, :, 0]
    total_hi = flat_totals.astype(bf16)
    total_left = flat_totals - total_hi.astype(f32)
    total_mid = total_left.astype(bf16)
    total_low = (total_left - total_mid.astype(f32)).astype(bf16)
    state_rows = prompts * DV
    sent = jnp.concatenate(
        [local.reshape(heads, state_rows, DK).astype(bf16), start_here, total_hi, total_mid, total_low], axis=1
    )
    moved = lax.all_gather(sent, "kv")
    all_local = moved[:, :, :state_rows].reshape(kv_size, heads, prompts, DV, DK)
    start_end = state_rows + start_here.shape[1]
    whole_start = moved[:, :, state_rows:start_end].reshape(kv_size, heads, prompts, rows_k, DV)
    whole_start = whole_start.transpose(1, 2, 4, 0, 3).reshape(heads, prompts, DV, DK).astype(f32)
    terms = moved[:, :, start_end:].reshape(kv_size, heads, 3, prompts, DK).astype(f32)
    all_totals = ((terms[:, :, 0] + terms[:, :, 1]) + terms[:, :, 2])[:, :, :, None]

    dec_all = dec_prod.reshape(2, PAD, -1)[:, :dec_own].reshape(2 * dec_own, -1)
    seqs = 2 * dec_own
    q_d = dec_all[:, :qk].reshape(seqs, heads, DK)
    k_d = dec_all[:, qk : 2 * qk].reshape(seqs, heads, DK)
    e_d = jnp.exp(dec_all[:, 2 * qk : 3 * qk]).reshape(seqs, heads, DK)
    qk_d = jnp.broadcast_to(jnp.sum(q_d * k_d, axis=-1, keepdims=True), q_d.shape)
    cols = jnp.concatenate([q_d * e_d, e_d, k_d, qk_d], axis=1).transpose(0, 2, 1)
    v_d = dec_all[:, 3 * qk :][:, None]
    dec_att, decode_out = pl.pallas_call(
        functools.partial(decode_kernel, heads),
        name="decode",
        grid=(seqs,),
        out_shape=(
            jax.ShapeDtypeStruct((seqs, 1, vw), f32),
            jax.ShapeDtypeStruct(decode_state.shape, f32),
        ),
        in_specs=[
            pl.BlockSpec((1, DK, 4 * heads), lambda i: (i, 0, 0)),
            pl.BlockSpec((1, 1, vw), lambda i: (i, 0, 0)),
            pl.BlockSpec((1, heads, DK, DV), lambda i: (i, 0, 0, 0)),
        ],
        out_specs=(
            pl.BlockSpec((1, 1, vw), lambda i: (i, 0, 0)),
            pl.BlockSpec((1, heads, DK, DV), lambda i: (i, 0, 0, 0)),
        ),
        cost_estimate=pl.CostEstimate(flops=8 * decode_state.size, bytes_accessed=8 * decode_state.size, transcendentals=0),
    )(cols, v_d, decode_state)

    running = whole_start
    incoming = whole_start
    for c in range(kv_size):
        incoming = jnp.where(kv_index == c, running, incoming)
        running = jnp.exp(all_totals[c]) * running + all_local[c].astype(f32)
    prompt_out = lax.dynamic_slice_in_dim(running, kv_index * rows_k, rows_k, 3).transpose(1, 0, 3, 2)

    dec_pad = jnp.pad(dec_att.reshape(2, dec_own, vw), ((0, 0), (0, PAD - dec_own), (0, 0))).reshape(2 * PAD, vw)
    y, yd = pl.pallas_call(
        functools.partial(back_kernel, own, chunk, prompts, heads),
        name="back",
        out_shape=(
            jax.ShapeDtypeStruct((own, w_out.shape[1]), bf16),
            jax.ShapeDtypeStruct((PAD, w_out.shape[1]), bf16),
        ),
        in_specs=[VMEM] * 5 + [ANY],
        out_specs=(VMEM,) * 2,
        scratch_shapes=[
            pltpu.VMEM(w_out.shape, bf16),
            pltpu.VMEM((rows, vw), bf16),
            pltpu.VMEM((own, vw), bf16),
            pltpu.VMEM((2 * PAD, vw), bf16),
            pltpu.VMEM((PAD, vw), bf16),
            pltpu.SemaphoreType.DMA,
            pltpu.SemaphoreType.DMA((count,)),
            pltpu.SemaphoreType.DMA((count,)),
            pltpu.SemaphoreType.DMA,
            pltpu.SemaphoreType.DMA,
        ],
        compiler_params=pltpu.CompilerParams(collective_id=1, has_side_effects=True, vmem_limit_bytes=LIMIT),
        cost_estimate=pl.CostEstimate(flops=2 * own * w_out.size, bytes_accessed=20_000_000, transcendentals=0),
    )(out_local, q_total, incoming.reshape(heads, prompts * DV, DK).astype(bf16), gain_here, dec_pad, w_out)
    return (y.reshape(own_pos, prompts, -1), yd[:dec_own], prompt_out, decode_out)


def solution(mesh):
    return jax.shard_map(
        on_device,
        mesh=mesh,
        in_specs=(
            P(("kv", "tp"), "dp", None),
            P(("dp", "kv", "tp"), None),
            P(None, "tp"),
            P(None, "tp"),
            P(None, "tp"),
            P(None, "tp"),
            P(),
            P(),
            P(),
            P(),
            P("dp", "tp", "kv", None),
            P(("dp", "kv"), "tp", None, None),
        ),
        out_specs=(
            P(("kv", "tp"), "dp", None),
            P(("dp", "kv", "tp"), None),
            P("dp", "tp", "kv", None),
            P(("dp", "kv"), "tp", None, None),
        ),
        check_vma=False,
    )
```
